32 devices in a mesh: kv: 8 (over z, y), tp: 4 (over x, core).
Axes of the slice: x: 2, y: 2, z: 4, core: 2. Of those that a mesh axis runs over, the one named last changes fastest.
Arguments:
- tokens: bfloat16 [4096, 2048], P('kv'), may hold values from -18 to 18
- w_query: bfloat16 [2048, 1024], P(None, 'tp'), may hold values from -0.125 to 0.125
- w_key: bfloat16 [2048, 256], P(None, 'tp'), may hold values from -0.125 to 0.125
- w_value: bfloat16 [2048, 256], P(None, 'tp'), may hold values from -18 to 18
- w_out: bfloat16 [1024, 2048], P(None, 'tp'), may hold values from -0.1875 to 0.1875
- out_gain: float32 [1024], replicated, may hold values from 0.1 to 1.9
- chosen: int32 [4, 64, 8], P('tp', 'kv'), may hold values from -1 to 63, as said below
Outputs:
- mixed_out: bfloat16 [4096, 2048], P('kv', 'tp')
The draws below stay inside these ranges and needn't reach their ends.
Inputs may be any that keep to these rules, and one draw needn't show every extreme that they name: chosen[h, b, 0] is b itself; the other entries of a row are distinct key blocks lying wholly before block b, or -1, placed after all named blocks; for each key head h, the query blocks on one index of kv (its 512 positions) name, together, at most one key block of head h held by any other index of kv.
All inputs are finite; a program needn't handle non-finite values.
Results may differ from the reference program's by a relative error of at most 0.024.
Values may be sent and summed in bfloat16 or wider, within the bound.
No kernel may reach another device: no remote copies, remote signals or barrier semaphores. Data moves between devices by JAX's collectives and lax.ppermute only.
A program may use at most 64 MiB of HBM per device.

```python
import jax
import jax.numpy as jnp
from jax import lax

D = 2048
HQ = 16
KVH = 4
HD = 64
BLK = 64
SEL = 8
TOK_DEV = 512
TOKENS = 4096
BLOCKS = 64
N_KV = 8


def draw_tokens(key, part):
    return jax.random.truncated_normal(key, -6.0, 6.0, (TOKENS, D), jnp.float32).astype(jnp.bfloat16)


def draw_w_value(key, part):
    column_head = (jnp.arange(KVH * HD, dtype=jnp.int32) // HD).astype(jnp.float32)
    fraction = column_head / (KVH - 1)
    entries = jax.random.truncated_normal(key, -6.0, 6.0, (D, KVH * HD), jnp.float32)
    factor = 3.0 ** fraction
    return (entries * factor[None, :] * D ** (-0.5)).astype(jnp.bfloat16)


def draw_chosen(key, part):
    per_device = TOK_DEV // BLK
    extra = SEL - 1
    rank_total = min(N_KV, per_device * extra)
    key_one, key_two = jax.random.split(key)
    owner_pick = jax.random.randint(key_one, (KVH, N_KV, N_KV), 0, per_device)
    noise = jax.random.randint(key_two, (KVH, N_KV, N_KV), 0, 1024)
    device_ids = jnp.arange(N_KV, dtype=jnp.int32)[:, None]
    owner_ids = jnp.arange(N_KV, dtype=jnp.int32)[None, :]
    below = owner_ids < device_ids
    forced = below & ((owner_ids == device_ids - 1) | (owner_ids == device_ids - N_KV // 2) | (owner_ids == 0))
    ranking = (noise + 2048 * forced.astype(jnp.int32)[None]) * N_KV + (N_KV - 1 - owner_ids)[None]
    ranking = jnp.where(below[None], ranking, -1)
    ignored, order = lax.top_k(ranking, rank_total)
    block_ids = jnp.arange(BLOCKS, dtype=jnp.int32)
    device = block_ids // per_device
    local_index = block_ids % per_device
    slot = jnp.arange(extra, dtype=jnp.int32)[None, :]
    remote_count = jnp.clip(device - local_index * extra, 0, extra)[:, None]
    rank = jnp.minimum(local_index[:, None] * extra + slot, rank_total - 1)
    order_rows = order[:, device, :]
    owner_sel = jnp.take_along_axis(order_rows, jnp.broadcast_to(rank[None], (KVH, BLOCKS, extra)), axis=2)
    head_index = jnp.arange(KVH, dtype=jnp.int32)[:, None, None]
    candidate = owner_pick[head_index, device[None, :, None], owner_sel]
    remote_block = owner_sel * per_device + candidate
    local_slot = slot - remote_count
    local_block = device[:, None] * per_device + local_slot
    fallback = jnp.where((local_slot >= 0) & (local_slot < local_index[:, None]), local_block, -1)
    picked = jnp.where((slot < remote_count)[None], remote_block, fallback[None])
    own_block = jnp.broadcast_to(block_ids[None, :, None], (KVH, BLOCKS, 1))
    return jnp.concatenate([own_block, picked], axis=2).astype(jnp.int32)


def block_scale(key, dims, cuts, least, high):
    def one(dim, parts):
        draws = jax.random.uniform(jax.random.fold_in(jax.random.fold_in(key, 6), dim), (parts,), jnp.float32, least / len(cuts), high / len(cuts))
        return jnp.repeat(jnp.exp(draws), dims[dim] // parts).reshape((-1,) + (1,) * (len(dims) - dim - 1))

    factor_of = one(*cuts[0])
    for cut in cuts[1:]:
        factor_of = factor_of * one(*cut)
    return factor_of


def centred(rng, shape, width, most, shards=(), held_as=jnp.bfloat16):
    loudness = block_scale(rng, shape, shards, -0.22, 0.18) if shards else 1.0
    result = jax.random.normal(rng, shape, jnp.float32) * width * loudness
    return jnp.minimum(jnp.maximum(result, -most), most).astype(held_as)


def setup_inputs(seed: int = 0) -> dict:
    key_list = jax.random.split(jax.random.key(seed), 8)
    return {
        "tokens": draw_tokens(jax.random.fold_in(key_list[7], 71), 0),
        "w_query": centred(key_list[1], (D, HQ * HD), D ** -0.5, 0.125, ((1, 4),)),
        "w_key": centred(key_list[2], (D, KVH * HD), D ** -0.5, 0.125, ((1, 4),)),
        "w_value": draw_w_value(jax.random.fold_in(key_list[7], 71), 0),
        "w_out": centred(key_list[4], (HQ * HD, D), (HQ * HD) ** -0.5, 0.1875, ((1, 4),)),
        "out_gain": jnp.clip(1.0 + 0.18 * jax.random.normal(key_list[5], (HQ * HD,), jnp.float32), 0.1, 1.9),
        "chosen": draw_chosen(jax.random.fold_in(key_list[7], 71), 0),
    }


rope_base = 500000.0
norm_eps = 1e-06

def rotate(vectors, positions):
    half_size = vectors.shape[-1] // 2
    frequency = rope_base ** (-jnp.arange(half_size, dtype=jnp.float32) / half_size)
    angles = positions.astype(jnp.float32)[:, None] * frequency[None, :]
    cosine = jnp.cos(angles)[:, None, :]
    sine_wave = jnp.sin(angles)[:, None, :]
    lower_half = vectors[..., :half_size]
    upper_half = vectors[..., half_size:]
    return jnp.concatenate([lower_half * cosine - upper_half * sine_wave, upper_half * cosine + lower_half * sine_wave], axis=-1)

def reference(tokens, w_query, w_key, w_value, w_out, out_gain, chosen):
    row_total = tokens.shape[0]
    positions = jnp.arange(row_total, dtype=jnp.int32)
    queries = rotate(jnp.dot(tokens, w_query, preferred_element_type=jnp.float32).reshape(row_total, HQ, HD), positions).astype(jnp.bfloat16)
    key_rows = rotate(jnp.dot(tokens, w_key, preferred_element_type=jnp.float32).reshape(row_total, KVH, HD), positions).astype(jnp.bfloat16)
    value_rows = jnp.dot(tokens, w_value, preferred_element_type=jnp.float32).astype(jnp.bfloat16).reshape(row_total, KVH, HD)
    block_total = row_total // BLK
    group_size = HQ // KVH
    key_blocks = key_rows.reshape(block_total, BLK, KVH, HD).transpose(2, 0, 1, 3)
    value_blocks = value_rows.reshape(block_total, BLK, KVH, HD).transpose(2, 0, 1, 3)
    query_blocks = queries.reshape(block_total, BLK, KVH, group_size, HD)
    head_rows = jnp.arange(KVH, dtype=jnp.int32)[:, None]
    offsets = jnp.arange(BLK, dtype=jnp.int32)
    score_scale = HD ** (-0.5)

    def attend(block_index):
        chosen_ids = chosen[:, block_index, :]
        usable = chosen_ids >= 0
        safe_ids = jnp.maximum(chosen_ids, 0)
        key_part = key_blocks[head_rows, safe_ids].astype(jnp.float32)
        value_part = value_blocks[head_rows, safe_ids].astype(jnp.float32)
        query_part = query_blocks[block_index].astype(jnp.float32)
        scores = jnp.einsum('qhgd,hskd->hgqsk', query_part, key_part) * score_scale
        key_pos = chosen_ids[:, :, None] * BLK + offsets
        query_pos = block_index * BLK + offsets
        allowed = usable[:, None, :, None] & (key_pos[:, None, :, :] <= query_pos[None, :, None, None])
        scores = jnp.where(allowed[:, None], scores, -jnp.inf)
        peak_score = lax.optimization_barrier(jnp.max(scores, axis=(3, 4), keepdims=True))
        weights = jnp.exp(scores - peak_score)
        weights = weights / lax.optimization_barrier(jnp.sum(weights, axis=(3, 4), keepdims=True))
        weights = lax.optimization_barrier(weights.astype(jnp.bfloat16)).astype(jnp.float32)
        mixed_out = jnp.einsum('hgqsk,hskd->qhgd', weights, value_part)
        return mixed_out.reshape(BLK, HQ * HD).astype(jnp.bfloat16)
    attended = lax.map(attend, jnp.arange(block_total, dtype=jnp.int32)).reshape(row_total, HQ * HD)
    attn_f32 = attended.astype(jnp.float32)
    squares = lax.optimization_barrier(jnp.sum(attn_f32 * attn_f32, axis=1))
    inverse = lax.rsqrt(squares / (HQ * HD) + norm_eps)
    scaled = (attn_f32 * out_gain[None, :]).astype(jnp.bfloat16)
    product = jnp.dot(scaled, w_out, preferred_element_type=jnp.float32)
    return (inverse[:, None] * product).astype(jnp.bfloat16)
```

```python
import functools

import jax
import jax.numpy as jnp
import numpy as np
from jax import lax
from jax.experimental import pallas as pl
from jax.experimental.pallas import tpu as pltpu
from jax.sharding import PartitionSpec as P

HD = 64
BLK = 64
LANES = 2 * HD
PAIR = 2 * BLK
CHUNKS = 2
ROPE_BASE = 500000.0
NORM_EPS = 1e-06
MASKED = -1e30
F32 = jnp.float32
BF16 = jnp.bfloat16


def rope_tables(rows, places):
    half = HD // 2
    frequency = ROPE_BASE ** (-np.arange(half, dtype=np.float64) / half)
    reps = LANES // half

    def both(positions):
        angles = positions[:, None].astype(np.float64) * frequency[None, :]
        wide = np.tile(angles, (1, reps))
        return np.cos(wide).astype(np.float32), np.sin(wide).astype(np.float32)

    row_cos, row_sin = both(np.arange(rows))
    place_cos, place_sin = both(np.arange(places) * rows)
    return row_cos, row_sin, np.concatenate([place_cos, place_sin], axis=1)


def vmem():
    return pl.BlockSpec(memory_space=pltpu.VMEM)


def call(kernel, outs, n_in, flops, scratch=(), mib=16, name=None):
    return pl.pallas_call(
        kernel,
        out_shape=outs,
        in_specs=[vmem()] * n_in,
        out_specs=jax.tree.map(lambda _: vmem(), outs),
        scratch_shapes=list(scratch),
        compiler_params=pltpu.CompilerParams(vmem_limit_bytes=mib * 2**20),
        cost_estimate=pl.CostEstimate(flops=flops, bytes_accessed=2**20, transcendentals=0),
        name=name,
    )


def lane_index(shape):
    return lax.broadcasted_iota(jnp.int32, shape, len(shape) - 1)


def cos_sin(cos_ref, sin_ref, place_ref):
    place = place_ref[pl.ds(lax.axis_index("kv"), 1), :]
    pc, ps = place[:, :LANES], place[:, LANES:]
    rc, rs = cos_ref[...], sin_ref[...]
    cosine = rc * pc - rs * ps
    sine = rs * pc + rc * ps
    first = lane_index(sine.shape) % HD < HD // 2
    return cosine, jnp.where(first, -sine, sine)


def turn(values, cosine, sine):
    first = lane_index(values.shape) % HD < HD // 2
    swapped = jnp.where(
        first, pltpu.roll(values, LANES - HD // 2, 1), pltpu.roll(values, HD // 2, 1)
    )
    return values * cosine + swapped * sine


def kv_kernel(x_ref, wk_ref, wv_ref, cos_ref, sin_ref, place_ref, out_ref, w_ref):
    w_ref[:HD, :] = wk_ref[...]
    w_ref[HD:, :] = wv_ref[...]
    both = lax.dot_general(
        x_ref[...], w_ref[...], (((1,), (1,)), ((), ())), preferred_element_type=F32
    )
    cosine, sine = cos_sin(cos_ref, sin_ref, place_ref)
    turned = turn(both, cosine, sine)
    out_ref[...] = jnp.where(lane_index(both.shape) < HD, turned, both).astype(BF16)


def pick_kernel(table_ref, pair_ref, out_ref):
    peers = table_ref.shape[0]
    blocks = pair_ref.shape[0] // BLK
    first = lax.axis_index("kv") * blocks

    def one(peer):
        local = table_ref[peer] - first
        mine = (local >= 0) & (local < blocks)
        index = jnp.max(jnp.where(mine, local, 0))
        out_ref[peer] = pair_ref[pl.ds(pl.multiple_of(index * BLK, BLK), BLK), :]

    if peers <= 16:
        for peer in range(peers):
            one(peer)
    else:
        pl.loop(0, peers)(one)


def heads_of(q, count):
    order = list(range(0, count, 2)) + list(range(1, count, 2))
    return jnp.concatenate([q[:, h * HD : (h + 1) * HD] for h in order], axis=0)


def value_forms(pairs):
    low = lane_index(pairs.shape) < HD
    one = jnp.ones((), BF16)
    wide = pairs.astype(F32)
    even = jnp.where(low, pltpu.roll(wide, HD, 1), 1.0).astype(BF16)
    odd = jnp.where(low, one, pairs)
    return even, odd


def attend(q, keys, even, odd, bias, rows, heads):
    stacked = heads_of(q, heads)
    scores = lax.dot_general(stacked, keys, (((1,), (1,)), ((), ())), preferred_element_type=F32)
    width = scores.shape[1]
    scores = (scores.reshape(heads, rows, width) + bias[None]).reshape(heads * rows, width)
    peak = jnp.max(scores, axis=1, keepdims=True)
    weights = jnp.exp(scores - peak).astype(BF16)
    split = heads // 2 * rows
    even_out = jnp.dot(weights[:split], even, preferred_element_type=F32)
    odd_out = jnp.dot(weights[split:], odd, preferred_element_type=F32)
    low = lane_index((rows, LANES)) < HD
    results = []
    for j in range(heads // 2):
        e = even_out[j * rows : (j + 1) * rows]
        o = odd_out[j * rows : (j + 1) * rows]
        total = jnp.where(low, e, o)
        sums = pltpu.roll(jnp.where(low, o, e), HD, 1)
        tops = jnp.where(
            low, peak[j * rows : (j + 1) * rows], peak[split + j * rows : split + (j + 1) * rows]
        )
        results.append((total, sums, tops))
    return results


def local_kernel(x_ref, w_ref, cos_ref, sin_ref, place_ref, pair_ref, ch_ref, *outs):
    q_ref, lse_ref, *o_refs = outs
    rows, width = q_ref.shape
    heads = width // HD
    blocks = rows // BLK
    q = jnp.dot(x_ref[...], w_ref[...], preferred_element_type=F32)
    cosine, sine = cos_sin(cos_ref, sin_ref, place_ref)
    for j in range(width // LANES):
        part = turn(q[:, j * LANES : (j + 1) * LANES], cosine, sine)
        q_ref[:, j * LANES : (j + 1) * LANES] = (part * HD**-0.5).astype(BF16)
    names = ch_ref[...]
    key_block = lane_index((blocks, rows)) // BLK + lax.axis_index("kv") * blocks
    named = names[:, 0:1] == key_block
    for s in range(1, names.shape[1]):
        named = named | (names[:, s : s + 1] == key_block)
    bias = jnp.where(named, 0.0, MASKED)
    per_chunk = rows // len(o_refs)
    pairs = pair_ref[...]
    even, odd = value_forms(pairs)
    for i in range(rows // PAIR):
        at, span = i * PAIR, (i + 1) * PAIR
        mask = jnp.concatenate(
            [
                jnp.broadcast_to(bias[2 * i + k : 2 * i + k + 1, :span], (BLK, span))
                for k in range(2)
            ],
            axis=0,
        )
        row = lax.broadcasted_iota(jnp.int32, (PAIR, span), 0) + at
        mask = jnp.where(lane_index((PAIR, span)) <= row, mask, MASKED)
        parts = attend(
            q_ref[at:span, :], pairs[:span, :HD], even[:span], odd[:span], mask, PAIR, heads
        )
        for j, (total, sums, tops) in enumerate(parts):
            lanes = slice(j * LANES, (j + 1) * LANES)
            lse_ref[at:span, lanes] = tops + jnp.log(sums)
            o_refs[at // per_chunk][at % per_chunk : at % per_chunk + PAIR, lanes] = (
                total / sums
            ).astype(BF16)


def remote_kernel(start, ch_ref, q_ref, lse_ref, arr_ref, o_ref, out_ref, seen_ref):
    rows, width = o_ref.shape
    heads = width // HD
    blocks = q_ref.shape[0] // BLK
    peers = arr_ref.shape[0] // BLK
    group = 8 if peers % 8 == 0 else peers
    span = group * BLK
    me = lax.axis_index("kv")
    names = ch_ref[...]
    owners = jnp.where(names >= 0, names // blocks, me)
    away = jnp.where(owners == me, -1, owners)
    out_ref[...] = o_ref[...]
    if peers > group:
        seen_ref[...] = lse_ref[start : start + rows, :]

    def block(b, base, bias, keys):
        first = start + b * BLK
        even, odd = value_forms(keys)
        parts = attend(
            q_ref[first : first + BLK, :], keys[:, :HD], even, odd, bias, BLK, heads
        )
        for j, (total, sums, tops) in enumerate(parts):
            at = (slice(first, first + BLK), slice(j * LANES, (j + 1) * LANES))
            here = (slice(b * BLK, (b + 1) * BLK), at[1])
            lse = seen_ref[here] if peers > group else lse_ref[at]
            top = jnp.maximum(lse, tops)
            old = jnp.exp(lse - top)
            new = jnp.exp(tops - top)
            both = old + sums * new
            mixed = (out_ref[here].astype(F32) * old + total * new) / both
            out_ref[here] = mixed.astype(BF16)
            if peers > group:
                seen_ref[here] = top + jnp.log(both)

    def one_group(g):
        base = g * group
        key_peer = lane_index((blocks, span)) // BLK + base
        named = away[:, 0:1] == key_peer
        for s in range(1, names.shape[1]):
            named = named | (away[:, s : s + 1] == key_peer)
        bias = jnp.where(named, 0.0, MASKED)
        for b in range(rows // BLK):
            row = bias[start // BLK + b : start // BLK + b + 1]
            used = jnp.max(row) > -1.0

            @pl.when(used)
            def _():
                keys = arr_ref[pl.ds(pl.multiple_of(base * BLK, span), span), :]
                block(b, base, jnp.broadcast_to(row, (BLK, span)), keys)

    if peers == group:
        one_group(0)
    else:
        pl.loop(0, peers // group)(one_group)


def out_kernel(columns, start, masks, *refs):
    *part_refs, gain_ref, w_ref, out_ref = refs[: len(masks) + 2] + refs[-1:]
    me = lax.axis_index("tp")
    width = part_refs[0].shape[1]
    squares = 0.0
    product = 0.0
    for mask, ref in zip(masks, part_refs, strict=True):
        at = pl.multiple_of((me ^ mask) * width, width)
        att = ref[...].astype(F32)
        squares = squares + jnp.sum(att * att, axis=1, keepdims=True)
        scaled = (att * gain_ref[:, pl.ds(at, width)]).astype(BF16)
        product = product + jnp.dot(
            scaled, w_ref[pl.ds(at, width), :], preferred_element_type=F32
        )
    inverse = lax.rsqrt(squares / columns + NORM_EPS)
    out_ref[...] = (inverse * product).astype(BF16)


def per_device(tables, tokens, w_query, w_key, w_value, w_out, out_gain, chosen):
    peers = lax.axis_size("kv")
    ways = lax.axis_size("tp")
    rows, depth = tokens.shape
    width = w_query.shape[1]
    names = chosen[0]
    row_cos, row_sin, place = (jnp.asarray(t) for t in tables)
    asked = lax.all_to_all(
        jnp.broadcast_to(names[None], (peers, *names.shape)), "kv", 0, 0, tiled=True
    )
    pairs = call(
        kv_kernel,
        jax.ShapeDtypeStruct((rows, LANES), BF16),
        6,
        2 * rows * depth * LANES,
        [pltpu.VMEM((LANES, depth), BF16)],
        name="kv",
    )(tokens, w_key.T, w_value.T, row_cos, row_sin, place)
    outgoing = call(
        pick_kernel, jax.ShapeDtypeStruct((peers, BLK, LANES), BF16), 2, 10**6, name="pick"
    )(asked, pairs)
    arrived = lax.all_to_all(outgoing, "kv", 0, 0, tiled=True).reshape(peers * BLK, LANES)
    step = rows // CHUNKS
    q, lse, *attended = call(
        local_kernel,
        (
            jax.ShapeDtypeStruct((rows, width), BF16),
            jax.ShapeDtypeStruct((rows, width), F32),
        )
        + tuple(jax.ShapeDtypeStruct((step, width), BF16) for _ in range(CHUNKS)),
        7,
        4 * rows * depth * width,
        mib=24,
        name="local",
    )(tokens, w_query, row_cos, row_sin, place, pairs, names)
    chunks = []
    for c in range(CHUNKS):
        mixed = call(
            functools.partial(remote_kernel, c * step),
            jax.ShapeDtypeStruct((step, width), BF16),
            5,
            10**8,
            [pltpu.VMEM((step, width) if peers > 8 else (8, LANES), F32)],
            name=f"remote{c}",
        )(names, q, lse, arrived, attended[c])
        held, masks = [mixed], [0]
        bit = ways // 2
        while bit:
            swap = [(i, i ^ bit) for i in range(ways)]
            held = held + [lax.ppermute(h, "tp", swap) for h in held]
            masks = masks + [m ^ bit for m in masks]
            bit //= 2
        chunks.append((held, tuple(masks)))
    gain = out_gain[None, :]
    columns = gain.shape[1]
    cols = w_out.shape[1]
    result = None
    for c, (held, masks) in enumerate(chunks):
        extra = [] if result is None else [result]
        result = pl.pallas_call(
            functools.partial(out_kernel, columns, c * step, masks),
            out_shape=jax.ShapeDtypeStruct((rows, cols), BF16),
            grid=(1,),
            in_specs=[vmem()] * (len(held) + 2) + [pl.BlockSpec(memory_space=pl.ANY)] * len(extra),
            out_specs=pl.BlockSpec((step, cols), lambda i, c=c: (c, 0)),
            input_output_aliases={len(held) + 2: 0} if extra else {},
            compiler_params=pltpu.CompilerParams(vmem_limit_bytes=16 * 2**20),
            cost_estimate=pl.CostEstimate(
                flops=2 * step * columns * cols, bytes_accessed=2**20, transcendentals=0
            ),
            name=f"out{c}",
        )(*held, gain, w_out, *extra)
    return result


def solution(mesh):
    def run(tokens, *rest):
        rows = tokens.shape[0] // mesh.shape["kv"]
        tables = rope_tables(rows, mesh.shape["kv"])
        return jax.shard_map(
            functools.partial(per_device, tables),
            mesh=mesh,
            in_specs=(
                P("kv", None),
                P(None, "tp"),
                P(None, "tp"),
                P(None, "tp"),
                P(None, "tp"),
                P(),
                P("tp", "kv", None),
            ),
            out_specs=P("kv", "tp"),
            check_vma=False,
        )(tokens, *rest)

    return run
```

```python
import functools

import jax
import jax.numpy as jnp
import numpy as np
from jax import lax
from jax.experimental import pallas as pl
from jax.experimental.pallas import tpu as pltpu
from jax.sharding import PartitionSpec as P


HD = 64
BLK = 64
LANES = 2 * HD
PAIR = 2 * BLK
CHUNKS = 2
SIGN_FLOPS = 10**10
ROPE_BASE = 500000.0
NORM_EPS = 1e-06
MASKED = -1e30
F32 = jnp.float32
BF16 = jnp.bfloat16


def rope_tables(rows, places):
    half = HD // 2
    frequency = ROPE_BASE ** (-np.arange(half, dtype=np.float64) / half)
    reps = LANES // half

    def both(positions):
        angles = positions[:, None].astype(np.float64) * frequency[None, :]
        wide = np.tile(angles, (1, reps))
        return np.cos(wide).astype(np.float32), np.sin(wide).astype(np.float32)

    row_cos, row_sin = both(np.arange(rows))
    place_cos, place_sin = both(np.arange(places) * rows)
    return row_cos, row_sin, np.concatenate([place_cos, place_sin], axis=1)


def vmem():
    return pl.BlockSpec(memory_space=pltpu.VMEM)


def call(kernel, outs, n_in, flops, scratch=(), mib=16):
    return pl.pallas_call(
        kernel,
        out_shape=outs,
        in_specs=[vmem()] * n_in,
        out_specs=jax.tree.map(lambda _: vmem(), outs),
        scratch_shapes=list(scratch),
        compiler_params=pltpu.CompilerParams(vmem_limit_bytes=mib * 2**20),
        cost_estimate=pl.CostEstimate(flops=flops, bytes_accessed=2**20, transcendentals=0),
    )


def lane_index(shape):
    return lax.broadcasted_iota(jnp.int32, shape, len(shape) - 1)


def cos_sin(cos_ref, sin_ref, place_ref, sign_ref):
    place = place_ref[pl.ds(lax.axis_index("kv"), 1), :]
    pc, ps = place[:, :LANES], place[:, LANES:]
    rc, rs = cos_ref[...], sin_ref[...]
    cosine = rc * pc - rs * ps
    sine = rs * pc + rc * ps
    return cosine, sine * sign_ref[0:1, :]


def turn(values, cosine, sine):
    first = lane_index(values.shape) % HD < HD // 2
    swapped = jnp.where(
        first, pltpu.roll(values, LANES - HD // 2, 1), pltpu.roll(values, HD // 2, 1)
    )
    return values * cosine + swapped * sine


def sign_kernel(out_ref):
    first = lane_index(out_ref.shape) % HD < HD // 2
    out_ref[...] = jnp.where(first, -1.0, 1.0)


def qkv_kernel(
    x_ref, wk_ref, wv_ref, wq_ref, cos_ref, sin_ref, place_ref, sign_ref, pair_ref, q_ref, wkv_ref
):
    wkv_ref[:HD, :] = wk_ref[...]
    wkv_ref[HD:, :] = wv_ref[...]
    both = lax.dot_general(
        x_ref[...], wkv_ref[...], (((1,), (1,)), ((), ())), preferred_element_type=F32
    )
    cosine, sine = cos_sin(cos_ref, sin_ref, place_ref, sign_ref)
    turned = turn(both, cosine, sine)
    pair_ref[...] = jnp.where(lane_index(both.shape) < HD, turned, both).astype(BF16)
    q = jnp.dot(x_ref[...], wq_ref[...], preferred_element_type=F32)
    for j in range(q_ref.shape[1] // LANES):
        lanes = slice(j * LANES, (j + 1) * LANES)
        q_ref[:, lanes] = (turn(q[:, lanes], cosine, sine) * HD**-0.5).astype(BF16)


def pick_kernel(masks, *refs):
    *table_refs, pair_ref, out_ref = refs
    blocks = pair_ref.shape[0] // BLK
    me = lax.axis_index("kv")
    first = me * blocks

    def one(peer, table):
        local = table - first
        mine = (local >= 0) & (local < blocks)
        index = jnp.max(jnp.where(mine, local, 0))
        out_ref[peer] = pair_ref[pl.ds(pl.multiple_of(index * BLK, BLK), BLK), :]

    if masks:
        out_ref[me] = pair_ref[:BLK, :]
        for ref, group in zip(table_refs, masks, strict=True):
            for i, mask in enumerate(group):
                one(me ^ mask, ref[i])
    else:
        pl.loop(0, out_ref.shape[0])(lambda peer: one(peer, table_refs[0][peer]))


def heads_of(q, count):
    order = list(range(0, count, 2)) + list(range(1, count, 2))
    return jnp.concatenate([q[:, h * HD : (h + 1) * HD] for h in order], axis=0)


def value_forms(pairs):
    low = lane_index(pairs.shape) < HD
    one = jnp.ones((), BF16)
    wide = pairs.astype(F32)
    even = jnp.where(low, pltpu.roll(wide, HD, 1), 1.0).astype(BF16)
    odd = jnp.where(low, one, pairs)
    return even, odd


def attend(q, keys, even, odd, bias, rows, heads):
    stacked = heads_of(q, heads)
    scores = lax.dot_general(stacked, keys, (((1,), (1,)), ((), ())), preferred_element_type=F32)
    width = scores.shape[1]
    scores = (scores.reshape(heads, rows, width) + bias[None]).reshape(heads * rows, width)
    peak = jnp.max(scores, axis=1, keepdims=True)
    weights = jnp.exp(scores - peak).astype(BF16)
    split = heads // 2 * rows
    even_out = jnp.dot(weights[:split], even, preferred_element_type=F32)
    odd_out = jnp.dot(weights[split:], odd, preferred_element_type=F32)
    low = lane_index((rows, LANES)) < HD
    results = []
    for j in range(heads // 2):
        e = even_out[j * rows : (j + 1) * rows]
        o = odd_out[j * rows : (j + 1) * rows]
        total = jnp.where(low, e, o)
        sums = pltpu.roll(jnp.where(low, o, e), HD, 1)
        tops = jnp.where(
            low, peak[j * rows : (j + 1) * rows], peak[split + j * rows : split + (j + 1) * rows]
        )
        results.append((total, sums, tops))
    return results


def local_kernel(q_ref, pair_ref, ch_ref, lse_ref, o_ref):
    rows, width = q_ref.shape
    heads = width // HD
    blocks = rows // BLK
    names = ch_ref[...]
    key_block = lane_index((blocks, rows)) // BLK + lax.axis_index("kv") * blocks
    named = names[:, 0:1] == key_block
    for s in range(1, names.shape[1]):
        named = named | (names[:, s : s + 1] == key_block)
    bias = jnp.where(named, 0.0, MASKED)
    pairs = pair_ref[...]
    even, odd = value_forms(pairs)
    for i in range(rows // PAIR):
        at, span = i * PAIR, (i + 1) * PAIR
        mask = jnp.concatenate(
            [
                jnp.broadcast_to(bias[2 * i + k : 2 * i + k + 1, :span], (BLK, span))
                for k in range(2)
            ],
            axis=0,
        )
        row = lax.broadcasted_iota(jnp.int32, (PAIR, span), 0) + at
        mask = jnp.where(lane_index((PAIR, span)) <= row, mask, MASKED)
        parts = attend(
            q_ref[at:span, :], pairs[:span, :HD], even[:span], odd[:span], mask, PAIR, heads
        )
        for j, (total, sums, tops) in enumerate(parts):
            lanes = slice(j * LANES, (j + 1) * LANES)
            lse_ref[at:span, lanes] = tops + jnp.log(sums)
            o_ref[at:span, lanes] = (total / sums).astype(BF16)


def remote_kernel(start, ch_ref, q_ref, lse_ref, arr_ref, o_ref, out_ref, seen_ref):
    rows, width = out_ref.shape
    heads = width // HD
    blocks = q_ref.shape[0] // BLK
    peers = arr_ref.shape[0] // BLK
    group = 8 if peers % 8 == 0 else peers
    span = group * BLK
    me = lax.axis_index("kv")
    names = ch_ref[...]
    owners = jnp.where(names >= 0, names // blocks, me)
    away = jnp.where(owners == me, -1, owners)
    out_ref[...] = o_ref[start : start + rows, :]
    if peers > group:
        seen_ref[...] = lse_ref[start : start + rows, :]

    def block(b, bias, keys):
        first = start + b * BLK
        even, odd = value_forms(keys)
        parts = attend(
            q_ref[first : first + BLK, :], keys[:, :HD], even, odd, bias, BLK, heads
        )
        for j, (total, sums, tops) in enumerate(parts):
            at = (slice(first, first + BLK), slice(j * LANES, (j + 1) * LANES))
            here = (slice(b * BLK, (b + 1) * BLK), at[1])
            lse = seen_ref[here] if peers > group else lse_ref[at]
            top = jnp.maximum(lse, tops)
            old = jnp.exp(lse - top)
            new = jnp.exp(tops - top)
            both = old + sums * new
            mixed = (out_ref[here].astype(F32) * old + total * new) / both
            out_ref[here] = mixed.astype(BF16)
            if peers > group:
                seen_ref[here] = top + jnp.log(both)

    def one_group(g):
        base = g * group
        key_peer = lane_index((blocks, span)) // BLK + base
        named = away[:, 0:1] == key_peer
        for s in range(1, names.shape[1]):
            named = named | (away[:, s : s + 1] == key_peer)
        bias = jnp.where(named, 0.0, MASKED)
        for b in range(rows // BLK):
            row = bias[start // BLK + b : start // BLK + b + 1]
            used = jnp.max(row) > -1.0

            @pl.when(used)
            def _():
                keys = arr_ref[pl.ds(pl.multiple_of(base * BLK, span), span), :]
                block(b, jnp.broadcast_to(row, (BLK, span)), keys)

    if peers == group:
        one_group(0)
    else:
        pl.loop(0, peers // group)(one_group)


def out_kernel(columns, masks, *refs):
    *part_refs, gain_ref, w_ref, out_ref = refs[: len(masks) + 2] + refs[-1:]
    me = lax.axis_index("tp")
    width = part_refs[0].shape[1]
    squares = 0.0
    product = 0.0
    for mask, ref in zip(masks, part_refs, strict=True):
        at = pl.multiple_of((me ^ mask) * width, width)
        att = ref[...].astype(F32)
        squares = squares + jnp.sum(att * att, axis=1, keepdims=True)
        scaled = (att * gain_ref[:, pl.ds(at, width)]).astype(BF16)
        product = product + jnp.dot(
            scaled, w_ref[pl.ds(at, width), :], preferred_element_type=F32
        )
    inverse = lax.rsqrt(squares / columns + NORM_EPS)
    out_ref[...] = (inverse * product).astype(BF16)


def per_device(tables, tokens, w_query, w_key, w_value, w_out, out_gain, chosen):
    peers = lax.axis_size("kv")
    ways = lax.axis_size("tp")
    rows, depth = tokens.shape
    width = w_query.shape[1]
    names = chosen[0]
    row_cos, row_sin, place = (jnp.asarray(t) for t in tables)
    swap = {}
    if peers <= 16 and peers & (peers - 1) == 0:
        swap = {m: [(i, i ^ m) for i in range(peers)] for m in range(1, peers)}
        beside = lax.ppermute(chosen, "kv", swap[1])
    else:
        table = jnp.broadcast_to(names[None], (peers, *names.shape))
        asked = [lax.all_to_all(table, "kv", 0, 0, tiled=True)]
        masks = ()
    sign = call(sign_kernel, jax.ShapeDtypeStruct((8, LANES), F32), 0, SIGN_FLOPS, mib=1)()
    pairs, q = call(
        qkv_kernel,
        (
            jax.ShapeDtypeStruct((rows, LANES), BF16),
            jax.ShapeDtypeStruct((rows, width), BF16),
        ),
        8,
        2 * rows * depth * (LANES + width),
        [pltpu.VMEM((LANES, depth), BF16)],
        mib=16,
    )(tokens, w_key.T, w_value.T, w_query, row_cos, row_sin, place, sign)
    if swap:
        beside, pairs, q = lax.optimization_barrier((beside, pairs, q))
        both = jnp.concatenate([chosen, beside], axis=0)
        asked = [beside] + [lax.ppermute(both, "kv", swap[m]) for m in range(2, peers, 2)]
        masks = ((1,),) + tuple((m, m ^ 1) for m in range(2, peers, 2))
    outgoing = call(
        functools.partial(pick_kernel, masks),
        jax.ShapeDtypeStruct((peers, BLK, LANES), BF16),
        len(asked) + 1,
        10**6,
        mib=4,
    )(*asked, pairs)
    arrived = lax.all_to_all(outgoing, "kv", 0, 0, tiled=True).reshape(peers * BLK, LANES)
    step = rows // CHUNKS
    lse, attended = call(
        local_kernel,
        (
            jax.ShapeDtypeStruct((rows, width), F32),
            jax.ShapeDtypeStruct((rows, width), BF16),
        ),
        3,
        2 * 10**9,
        mib=16,
    )(q, pairs, names)
    flips = [1 << i for i in reversed(range((ways - 1).bit_length()))]
    swaps = {m: [(i, i ^ m) for i in range(ways)] for m in flips}
    gain = out_gain[None, :]
    columns = gain.shape[1]
    cols = w_out.shape[1]
    sent = []
    for c in range(CHUNKS):
        mixed = call(
            functools.partial(remote_kernel, c * step),
            jax.ShapeDtypeStruct((step, width), BF16),
            5,
            10**8,
            [pltpu.VMEM((step, width) if peers > 8 else (8, LANES), F32)],
        )(names, q, lse, arrived, attended)
        sent.append([mixed, lax.ppermute(mixed, "tp", swaps[flips[0]])])
    result = None
    for c, held in enumerate(sent):
        masks = [0, flips[0]]
        for m in flips[1:]:
            more = []
            for h in held:
                more.append(lax.ppermute(h, "tp", swaps[m]))
            held = held + more
            masks = masks + [k ^ m for k in masks]
        extra = [] if result is None else [result]
        result = pl.pallas_call(
            functools.partial(out_kernel, columns, masks),
            out_shape=jax.ShapeDtypeStruct((rows, cols), BF16),
            grid=(1,),
            in_specs=[vmem()] * (len(held) + 2)
            + [pl.BlockSpec(memory_space=pl.ANY)] * len(extra),
            out_specs=pl.BlockSpec((step, cols), lambda i, c=c: (c, 0)),
            input_output_aliases={len(held) + 2: 0} if extra else {},
            compiler_params=pltpu.CompilerParams(vmem_limit_bytes=16 * 2**20),
            cost_estimate=pl.CostEstimate(
                flops=2 * step * columns * cols, bytes_accessed=2**20, transcendentals=0
            ),
        )(*held, gain, w_out, *extra)
    return result


def solution(mesh):
    def run(tokens, *rest):
        rows = tokens.shape[0] // mesh.shape["kv"]
        tables = rope_tables(rows, mesh.shape["kv"])

        def body(*args):
            return per_device(tables, *args)

        return jax.shard_map(
            body,
            mesh=mesh,
            in_specs=(
                P("kv", None),
                P(None, "tp"),
                P(None, "tp"),
                P(None, "tp"),
                P(None, "tp"),
                P(),
                P("tp", "kv", None),
            ),
            out_specs=P("kv", "tp"),
            check_vma=False,
        )(tokens, *rest)

    return run
```

```python
import functools

import jax
import jax.numpy as jnp
import numpy as np
from jax import lax
from jax.experimental import pallas as pl
from jax.experimental.pallas import tpu as pltpu
from jax.sharding import PartitionSpec as P


HD = 64
BLK = 64
LANES = 2 * HD
PAIR = 2 * BLK
CHUNKS = 2
SIGN_FLOPS = 10**10
ROPE_BASE = 500000.0
NORM_EPS = 1e-06
MASKED = -1e30
F32 = jnp.float32
BF16 = jnp.bfloat16


def rope_tables(rows, places):
    half = HD // 2
    frequency = ROPE_BASE ** (-np.arange(half, dtype=np.float64) / half)
    reps = LANES // half

    def both(positions):
        angles = positions[:, None].astype(np.float64) * frequency[None, :]
        wide = np.tile(angles, (1, reps))
        return np.cos(wide).astype(np.float32), np.sin(wide).astype(np.float32)

    row_cos, row_sin = both(np.arange(rows))
    place_cos, place_sin = both(np.arange(places) * rows)
    return row_cos, row_sin, np.concatenate([place_cos, place_sin], axis=1)


def vmem():
    return pl.BlockSpec(memory_space=pltpu.VMEM)


def call(kernel, outs, n_in, flops, scratch=(), mib=16):
    return pl.pallas_call(
        kernel,
        out_shape=outs,
        in_specs=[vmem()] * n_in,
        out_specs=jax.tree.map(lambda _: vmem(), outs),
        scratch_shapes=list(scratch),
        compiler_params=pltpu.CompilerParams(vmem_limit_bytes=mib * 2**20),
        cost_estimate=pl.CostEstimate(flops=flops, bytes_accessed=2**20, transcendentals=0),
    )


def lane_index(shape):
    return lax.broadcasted_iota(jnp.int32, shape, len(shape) - 1)


def cos_sin(cos_ref, sin_ref, place_ref, sign_ref):
    place = place_ref[pl.ds(lax.axis_index("kv"), 1), :]
    pc, ps = place[:, :LANES], place[:, LANES:]
    rc, rs = cos_ref[...], sin_ref[...]
    cosine = rc * pc - rs * ps
    sine = rs * pc + rc * ps
    return cosine, sine * sign_ref[0:1, :]


def turn(values, cosine, sine):
    first = lane_index(values.shape) % HD < HD // 2
    swapped = jnp.where(
        first, pltpu.roll(values, LANES - HD // 2, 1), pltpu.roll(values, HD // 2, 1)
    )
    return values * cosine + swapped * sine


def sign_kernel(out_ref):
    first = lane_index(out_ref.shape) % HD < HD // 2
    out_ref[...] = jnp.where(first, -1.0, 1.0)


def qkv_kernel(
    x_ref, wk_ref, wv_ref, wq_ref, cos_ref, sin_ref, place_ref, sign_ref, pair_ref, q_ref, wkv_ref
):
    wkv_ref[:HD, :] = wk_ref[...]
    wkv_ref[HD:, :] = wv_ref[...]
    both = lax.dot_general(
        x_ref[...], wkv_ref[...], (((1,), (1,)), ((), ())), preferred_element_type=F32
    )
    cosine, sine = cos_sin(cos_ref, sin_ref, place_ref, sign_ref)
    turned = turn(both, cosine, sine)
    pair_ref[...] = jnp.where(lane_index(both.shape) < HD, turned, both).astype(BF16)
    q = jnp.dot(x_ref[...], wq_ref[...], preferred_element_type=F32)
    for j in range(q_ref.shape[1] // LANES):
        lanes = slice(j * LANES, (j + 1) * LANES)
        q_ref[:, lanes] = (turn(q[:, lanes], cosine, sine) * HD**-0.5).astype(BF16)


def pick_kernel(masks, *refs):
    *table_refs, pair_ref, out_ref = refs
    blocks = pair_ref.shape[0] // BLK
    me = lax.axis_index("kv")
    first = me * blocks

    def one(peer, table):
        local = table - first
        mine = (local >= 0) & (local < blocks)
        index = jnp.max(jnp.where(mine, local, 0))
        out_ref[peer] = pair_ref[pl.ds(pl.multiple_of(index * BLK, BLK), BLK), :]

    if masks:
        out_ref[me] = pair_ref[:BLK, :]
        for ref, group in zip(table_refs, masks, strict=True):
            for i, mask in enumerate(group):
                one(me ^ mask, ref[i])
    else:
        pl.loop(0, out_ref.shape[0])(lambda peer: one(peer, table_refs[0][peer]))


def heads_of(q, count):
    order = list(range(0, count, 2)) + list(range(1, count, 2))
    return jnp.concatenate([q[:, h * HD : (h + 1) * HD] for h in order], axis=0)


def value_forms(pairs):
    low = lane_index(pairs.shape) < HD
    one = jnp.ones((), BF16)
    wide = pairs.astype(F32)
    even = jnp.where(low, pltpu.roll(wide, HD, 1), 1.0).astype(BF16)
    odd = jnp.where(low, one, pairs)
    return even, odd


def attend(q, keys, even, odd, bias, rows, heads):
    stacked = heads_of(q, heads)
    scores = lax.dot_general(stacked, keys, (((1,), (1,)), ((), ())), preferred_element_type=F32)
    width = scores.shape[1]
    scores = (scores.reshape(heads, rows, width) + bias[None]).reshape(heads * rows, width)
    peak = jnp.max(scores, axis=1, keepdims=True)
    weights = jnp.exp(scores - peak).astype(BF16)
    split = heads // 2 * rows
    even_out = jnp.dot(weights[:split], even, preferred_element_type=F32)
    odd_out = jnp.dot(weights[split:], odd, preferred_element_type=F32)
    low = lane_index((rows, LANES)) < HD
    results = []
    for j in range(heads // 2):
        e = even_out[j * rows : (j + 1) * rows]
        o = odd_out[j * rows : (j + 1) * rows]
        total = jnp.where(low, e, o)
        sums = pltpu.roll(jnp.where(low, o, e), HD, 1)
        tops = jnp.where(
            low, peak[j * rows : (j + 1) * rows], peak[split + j * rows : split + (j + 1) * rows]
        )
        results.append((total, sums, tops))
    return results


def local_kernel(q_ref, pair_ref, ch_ref, lse_ref, o_ref):
    rows, width = q_ref.shape
    heads = width // HD
    blocks = rows // BLK
    names = ch_ref[...]
    key_block = lane_index((blocks, rows)) // BLK + lax.axis_index("kv") * blocks
    named = names[:, 0:1] == key_block
    for s in range(1, names.shape[1]):
        named = named | (names[:, s : s + 1] == key_block)
    bias = jnp.where(named, 0.0, MASKED)
    pairs = pair_ref[...]
    even, odd = value_forms(pairs)
    for i in range(rows // PAIR):
        at, span = i * PAIR, (i + 1) * PAIR
        mask = jnp.concatenate(
            [
                jnp.broadcast_to(bias[2 * i + k : 2 * i + k + 1, :span], (BLK, span))
                for k in range(2)
            ],
            axis=0,
        )
        row = lax.broadcasted_iota(jnp.int32, (PAIR, span), 0) + at
        mask = jnp.where(lane_index((PAIR, span)) <= row, mask, MASKED)
        parts = attend(
            q_ref[at:span, :], pairs[:span, :HD], even[:span], odd[:span], mask, PAIR, heads
        )
        for j, (total, sums, tops) in enumerate(parts):
            lanes = slice(j * LANES, (j + 1) * LANES)
            lse_ref[at:span, lanes] = tops + jnp.log(sums)
            o_ref[at:span, lanes] = (total / sums).astype(BF16)


def remote_kernel(start, ch_ref, q_ref, lse_ref, arr_ref, o_ref, out_ref, seen_ref):
    rows, width = out_ref.shape
    heads = width // HD
    blocks = q_ref.shape[0] // BLK
    peers = arr_ref.shape[0] // BLK
    group = 8 if peers % 8 == 0 else peers
    span = group * BLK
    me = lax.axis_index("kv")
    names = ch_ref[...]
    owners = jnp.where(names >= 0, names // blocks, me)
    away = jnp.where(owners == me, -1, owners)
    out_ref[...] = o_ref[start : start + rows, :]
    if peers > group:
        seen_ref[...] = lse_ref[start : start + rows, :]

    def block(b, bias, keys):
        first = start + b * BLK
        even, odd = value_forms(keys)
        parts = attend(
            q_ref[first : first + BLK, :], keys[:, :HD], even, odd, bias, BLK, heads
        )
        for j, (total, sums, tops) in enumerate(parts):
            at = (slice(first, first + BLK), slice(j * LANES, (j + 1) * LANES))
            here = (slice(b * BLK, (b + 1) * BLK), at[1])
            lse = seen_ref[here] if peers > group else lse_ref[at]
            top = jnp.maximum(lse, tops)
            old = jnp.exp(lse - top)
            new = jnp.exp(tops - top)
            both = old + sums * new
            mixed = (out_ref[here].astype(F32) * old + total * new) / both
            out_ref[here] = mixed.astype(BF16)
            if peers > group:
                seen_ref[here] = top + jnp.log(both)

    def one_group(g):
        base = g * group
        key_peer = lane_index((blocks, span)) // BLK + base
        named = away[:, 0:1] == key_peer
        for s in range(1, names.shape[1]):
            named = named | (away[:, s : s + 1] == key_peer)
        bias = jnp.where(named, 0.0, MASKED)
        for b in range(rows // BLK):
            row = bias[start // BLK + b : start // BLK + b + 1]
            used = jnp.max(row) > -1.0

            @pl.when(used)
            def _():
                keys = arr_ref[pl.ds(pl.multiple_of(base * BLK, span), span), :]
                block(b, jnp.broadcast_to(row, (BLK, span)), keys)

    if peers == group:
        one_group(0)
    else:
        pl.loop(0, peers // group)(one_group)


def out_kernel(columns, masks, *refs):
    *part_refs, gain_ref, w_ref, out_ref = refs[: len(masks) + 2] + refs[-1:]
    me = lax.axis_index("tp")
    width = part_refs[0].shape[1]
    squares = 0.0
    product = 0.0
    for mask, ref in zip(masks, part_refs, strict=True):
        at = pl.multiple_of((me ^ mask) * width, width)
        att = ref[...].astype(F32)
        squares = squares + jnp.sum(att * att, axis=1, keepdims=True)
        scaled = (att * gain_ref[:, pl.ds(at, width)]).astype(BF16)
        product = product + jnp.dot(
            scaled, w_ref[pl.ds(at, width), :], preferred_element_type=F32
        )
    inverse = lax.rsqrt(squares / columns + NORM_EPS)
    out_ref[...] = (inverse * product).astype(BF16)


def per_device(tables, tokens, w_query, w_key, w_value, w_out, out_gain, chosen):
    peers = lax.axis_size("kv")
    ways = lax.axis_size("tp")
    rows, depth = tokens.shape
    width = w_query.shape[1]
    names = chosen[0]
    row_cos, row_sin, place = (jnp.asarray(t) for t in tables)
    sign = call(sign_kernel, jax.ShapeDtypeStruct((8, LANES), F32), 0, SIGN_FLOPS, mib=1)()
    if spread(peers):
        swap = {m: [(i, i ^ m) for i in range(peers)] for m in range(1, peers)}
        beside = lax.ppermute(chosen, "kv", swap[1])
        both = jnp.concatenate([chosen, beside], axis=0)
        asked, masks = [beside], [(1,)]
        for m in range(peers - 2, 0, -2):
            asked.append(lax.ppermute(both, "kv", swap[m]))
            masks.append((m, m ^ 1))
    else:
        table = jnp.broadcast_to(names[None], (peers, *names.shape))
        asked = [lax.all_to_all(table, "kv", 0, 0, tiled=True)]
        masks = []
    pairs, q = call(
        qkv_kernel,
        (
            jax.ShapeDtypeStruct((rows, LANES), BF16),
            jax.ShapeDtypeStruct((rows, width), BF16),
        ),
        8,
        2 * rows * depth * (LANES + width),
        [pltpu.VMEM((LANES, depth), BF16)],
        mib=16,
    )(tokens, w_key.T, w_value.T, w_query, row_cos, row_sin, place, sign)
    outgoing = call(
        functools.partial(pick_kernel, masks),
        jax.ShapeDtypeStruct((peers, BLK, LANES), BF16),
        len(asked) + 1,
        10**6,
        mib=4,
    )(*asked, pairs)
    arrived = lax.all_to_all(outgoing, "kv", 0, 0, tiled=True).reshape(peers * BLK, LANES)
    step = rows // CHUNKS
    lse, attended = call(
        local_kernel,
        (
            jax.ShapeDtypeStruct((rows, width), F32),
            jax.ShapeDtypeStruct((rows, width), BF16),
        ),
        3,
        2 * 10**9,
        mib=16,
    )(q, pairs, names)
    flips = [1 << i for i in reversed(range((ways - 1).bit_length()))]
    swaps = {m: [(i, i ^ m) for i in range(ways)] for m in flips}
    gain = out_gain[None, :]
    columns = gain.shape[1]
    cols = w_out.shape[1]
    sent = []
    for c in reversed(range(CHUNKS)):
        mixed = call(
            functools.partial(remote_kernel, c * step),
            jax.ShapeDtypeStruct((step, width), BF16),
            5,
            10**8,
            [pltpu.VMEM((step, width) if peers > 8 else (8, LANES), F32)],
        )(names, q, lse, arrived, attended)
        sent.append((c, [mixed, lax.ppermute(mixed, "tp", swaps[flips[0]])]))
    result = None
    for c, held in sent:
        masks = [0, flips[0]]
        for m in flips[1:]:
            more = []
            for h in held:
                more.append(lax.ppermute(h, "tp", swaps[m]))
            held = held + more
            masks = masks + [k ^ m for k in masks]
        extra = [] if result is None else [result]
        result = pl.pallas_call(
            functools.partial(out_kernel, columns, masks),
            out_shape=jax.ShapeDtypeStruct((rows, cols), BF16),
            grid=(1,),
            in_specs=[vmem()] * (len(held) + 2)
            + [pl.BlockSpec(memory_space=pl.ANY)] * len(extra),
            out_specs=pl.BlockSpec((step, cols), lambda i, c=c: (c, 0)),
            input_output_aliases={len(held) + 2: 0} if extra else {},
            compiler_params=pltpu.CompilerParams(vmem_limit_bytes=16 * 2**20),
            cost_estimate=pl.CostEstimate(
                flops=2 * step * columns * cols, bytes_accessed=2**20, transcendentals=0
            ),
        )(*held, gain, w_out, *extra)
    return result


def spread(peers):
    return peers <= 16 and peers & (peers - 1) == 0


def solution(mesh):
    def run(tokens, *rest):
        rows = tokens.shape[0] // mesh.shape["kv"]
        tables = rope_tables(rows, mesh.shape["kv"])

        def body(*args):
            return per_device(tables, *args)

        return jax.shard_map(
            body,
            mesh=mesh,
            in_specs=(
                P("kv", None),
                P(None, "tp"),
                P(None, "tp"),
                P(None, "tp"),
                P(None, "tp"),
                P(),
                P("tp", "kv", None),
            ),
            out_specs=P("kv", "tp"),
            check_vma=False,
        )(tokens, *rest)

    return run
```

```python
import functools

import jax
import jax.numpy as jnp
import numpy as np
from jax import lax
from jax.experimental import pallas as pl
from jax.experimental.pallas import tpu as pltpu
from jax.sharding import PartitionSpec as P


HD = 64
BLK = 64
LANES = 2 * HD
PAIR = 2 * BLK
CHUNKS = 2
SIGN_FLOPS = 10**10
ROPE_BASE = 500000.0
NORM_EPS = 1e-06
MASKED = -1e30
F32 = jnp.float32
BF16 = jnp.bfloat16


def rope_tables(rows, places):
    half = HD // 2
    frequency = ROPE_BASE ** (-np.arange(half, dtype=np.float64) / half)

    def packed(positions):
        angles = positions[:, None].astype(np.float64) * frequency[None, :]
        pair = np.concatenate([np.cos(angles), np.sin(angles)], axis=1)
        return np.tile(pair, (1, LANES // HD)).astype(np.float32)

    return packed(np.arange(rows)), packed(np.arange(places) * rows)


def vmem():
    return pl.BlockSpec(memory_space=pltpu.VMEM)


def call(kernel, outs, n_in, flops, scratch=(), mib=16):
    return pl.pallas_call(
        kernel,
        out_shape=outs,
        in_specs=[vmem()] * n_in,
        out_specs=jax.tree.map(lambda _: vmem(), outs),
        scratch_shapes=list(scratch),
        compiler_params=pltpu.CompilerParams(vmem_limit_bytes=mib * 2**20),
        cost_estimate=pl.CostEstimate(flops=flops, bytes_accessed=2**20, transcendentals=0),
    )


def lane_index(shape):
    return lax.broadcasted_iota(jnp.int32, shape, len(shape) - 1)


def cos_sin(row_ref, place_ref, sign_ref):
    half = HD // 2

    def unpack(packed):
        low = lane_index(packed.shape) % HD < half
        cosine = jnp.where(low, packed, pltpu.roll(packed, half, 1))
        sine = jnp.where(low, pltpu.roll(packed, LANES - half, 1), packed)
        return cosine, sine

    rc, rs = unpack(row_ref[...])
    place = place_ref[pl.ds(lax.axis_index("kv"), 1), :]
    pc, ps = unpack(jnp.broadcast_to(place, (8, LANES)))
    pc, ps = pc[0:1], ps[0:1]
    return rc * pc - rs * ps, (rs * pc + rc * ps) * sign_ref[0:1, :]


def turn(values, cosine, sine):
    first = lane_index(values.shape) % HD < HD // 2
    swapped = jnp.where(
        first, pltpu.roll(values, LANES - HD // 2, 1), pltpu.roll(values, HD // 2, 1)
    )
    return values * cosine + swapped * sine


def sign_kernel(out_ref):
    first = lane_index(out_ref.shape) % HD < HD // 2
    out_ref[...] = jnp.where(first, -1.0, 1.0)


def kv_kernel(x_ref, wk_ref, wv_ref, row_ref, place_ref, sign_ref, pair_ref, wkv_ref):
    wkv_ref[:HD, :] = wk_ref[...]
    wkv_ref[HD:, :] = wv_ref[...]
    both = lax.dot_general(
        x_ref[...], wkv_ref[...], (((1,), (1,)), ((), ())), preferred_element_type=F32
    )
    cosine, sine = cos_sin(row_ref, place_ref, sign_ref)
    turned = turn(both, cosine, sine)
    pair_ref[...] = jnp.where(lane_index(both.shape) < HD, turned, both).astype(BF16)


def query_kernel(x_ref, wq_ref, row_ref, place_ref, sign_ref, q_ref):
    q = jnp.dot(x_ref[...], wq_ref[...], preferred_element_type=F32)
    cosine, sine = cos_sin(row_ref, place_ref, sign_ref)
    for j in range(q_ref.shape[1] // LANES):
        lanes = slice(j * LANES, (j + 1) * LANES)
        q_ref[:, lanes] = (turn(q[:, lanes], cosine, sine) * HD**-0.5).astype(BF16)


def wanted(table, owner, blocks):
    local = table - owner * blocks
    mine = (local >= 0) & (local < blocks)
    index = jnp.max(jnp.where(mine, local, 0))
    return pl.ds(pl.multiple_of(index * BLK, BLK), BLK)


def give_kernel(*refs):
    count = (len(refs) - 2) // 2
    table_refs, (pair_ref, beside_ref), out_refs = refs[:count], refs[count : count + 2], refs[count + 2 :]
    blocks = pair_ref.shape[0] // BLK
    me = lax.axis_index("kv")
    odd = me & 1
    for table_ref, out_ref in zip(table_refs, out_refs, strict=True):
        table = table_ref[0]
        for owner, ref in ((me, pair_ref), (me ^ 1, beside_ref)):
            place = odd if ref is pair_ref else 1 - odd
            at = pl.ds(pl.multiple_of(place * BLK, BLK), BLK)
            out_ref[at, :] = ref[wanted(table, owner, blocks), :]


def pick_kernel(table_ref, pair_ref, out_ref):
    blocks = pair_ref.shape[0] // BLK
    me = lax.axis_index("kv")

    def one(peer):
        out_ref[peer] = pair_ref[wanted(table_ref[peer], me, blocks), :]

    pl.loop(0, out_ref.shape[0])(one)


def heads_of(q, count):
    order = list(range(0, count, 2)) + list(range(1, count, 2))
    return jnp.concatenate([q[:, h * HD : (h + 1) * HD] for h in order], axis=0)


def value_forms(pairs):
    low = lane_index(pairs.shape) < HD
    one = jnp.ones((), BF16)
    wide = pairs.astype(F32)
    even = jnp.where(low, pltpu.roll(wide, HD, 1), 1.0).astype(BF16)
    odd = jnp.where(low, one, pairs)
    return even, odd


def attend(q, keys, even, odd, bias, rows, heads):
    stacked = heads_of(q, heads)
    scores = lax.dot_general(stacked, keys, (((1,), (1,)), ((), ())), preferred_element_type=F32)
    width = scores.shape[1]
    scores = (scores.reshape(heads, rows, width) + bias[None]).reshape(heads * rows, width)
    peak = jnp.max(scores, axis=1, keepdims=True)
    weights = jnp.exp(scores - peak).astype(BF16)
    split = heads // 2 * rows
    even_out = jnp.dot(weights[:split], even, preferred_element_type=F32)
    odd_out = jnp.dot(weights[split:], odd, preferred_element_type=F32)
    low = lane_index((rows, LANES)) < HD
    results = []
    for j in range(heads // 2):
        e = even_out[j * rows : (j + 1) * rows]
        o = odd_out[j * rows : (j + 1) * rows]
        total = jnp.where(low, e, o)
        sums = pltpu.roll(jnp.where(low, o, e), HD, 1)
        tops = jnp.where(
            low, peak[j * rows : (j + 1) * rows], peak[split + j * rows : split + (j + 1) * rows]
        )
        results.append((total, sums, tops))
    return results


def local_kernel(q_ref, pair_ref, ch_ref, lse_ref, o_ref):
    rows, width = q_ref.shape
    heads = width // HD
    blocks = rows // BLK
    names = ch_ref[...]
    key_block = lane_index((blocks, rows)) // BLK + lax.axis_index("kv") * blocks
    named = names[:, 0:1] == key_block
    for s in range(1, names.shape[1]):
        named = named | (names[:, s : s + 1] == key_block)
    bias = jnp.where(named, 0.0, MASKED)
    pairs = pair_ref[...]
    even, odd = value_forms(pairs)
    for i in range(rows // PAIR):
        at, span = i * PAIR, (i + 1) * PAIR
        mask = jnp.concatenate(
            [
                jnp.broadcast_to(bias[2 * i + k : 2 * i + k + 1, :span], (BLK, span))
                for k in range(2)
            ],
            axis=0,
        )
        row = lax.broadcasted_iota(jnp.int32, (PAIR, span), 0) + at
        mask = jnp.where(lane_index((PAIR, span)) <= row, mask, MASKED)
        parts = attend(
            q_ref[at:span, :], pairs[:span, :HD], even[:span], odd[:span], mask, PAIR, heads
        )
        for j, (total, sums, tops) in enumerate(parts):
            lanes = slice(j * LANES, (j + 1) * LANES)
            lse_ref[at:span, lanes] = tops + jnp.log(sums)
            o_ref[at:span, lanes] = (total / sums).astype(BF16)


def remote_kernel(start, masks, ch_ref, q_ref, lse_ref, o_ref, *refs):
    *key_refs, out_ref, seen_ref = refs
    rows, width = out_ref.shape
    heads = width // HD
    blocks = q_ref.shape[0] // BLK
    peers = sum(ref.shape[0] for ref in key_refs) // BLK
    group = peers if masks else 8
    span = group * BLK
    me = lax.axis_index("kv")
    names = ch_ref[...]
    owners = jnp.where(names >= 0, names // blocks, me)
    away = jnp.where(owners == me, -1, owners)
    out_ref[...] = o_ref[start : start + rows, :]
    if peers > group:
        seen_ref[...] = lse_ref[start : start + rows, :]

    def block(b, bias, keys):
        first = start + b * BLK
        even, odd = value_forms(keys)
        parts = attend(
            q_ref[first : first + BLK, :], keys[:, :HD], even, odd, bias, BLK, heads
        )
        for j, (total, sums, tops) in enumerate(parts):
            at = (slice(first, first + BLK), slice(j * LANES, (j + 1) * LANES))
            here = (slice(b * BLK, (b + 1) * BLK), at[1])
            lse = seen_ref[here] if peers > group else lse_ref[at]
            top = jnp.maximum(lse, tops)
            old = jnp.exp(lse - top)
            new = jnp.exp(tops - top)
            both = old + sums * new
            mixed = (out_ref[here].astype(F32) * old + total * new) / both
            out_ref[here] = mixed.astype(BF16)
            if peers > group:
                seen_ref[here] = top + jnp.log(both)

    def one_group(g):
        base = g * group
        key_peer = lane_index((blocks, span)) // BLK
        if masks:
            part = key_peer // 2
            column = jnp.full(part.shape, me & -2, jnp.int32)
            for i, mask in enumerate(masks):
                column = jnp.where(part == i, (me ^ mask) & -2, column)
            key_peer = column + key_peer % 2
        else:
            key_peer = key_peer + base
        named = away[:, 0:1] == key_peer
        for s in range(1, names.shape[1]):
            named = named | (away[:, s : s + 1] == key_peer)
        bias = jnp.where(named, 0.0, MASKED)
        inside = (away >= base) & (away < base + group)
        place = lax.broadcasted_iota(jnp.int32, away.shape, 0)
        flags = jnp.max(jnp.where(inside, 1 << place, 0), axis=1, keepdims=True)
        used = jnp.sum(flags)
        for b in range(rows // BLK):
            row = bias[start // BLK + b : start // BLK + b + 1]

            @pl.when((used >> (start // BLK + b)) & 1 == 1)
            def _():
                if masks:
                    keys = jnp.concatenate([ref[...] for ref in key_refs], axis=0)
                else:
                    keys = key_refs[0][pl.ds(pl.multiple_of(base * BLK, span), span), :]
                block(b, jnp.broadcast_to(row, (BLK, span)), keys)

    if peers == group:
        one_group(0)
    else:
        pl.loop(0, peers // group)(one_group)


def out_kernel(columns, masks, *refs):
    *part_refs, gain_ref, w_ref, out_ref = refs[: len(masks) + 2] + refs[-1:]
    me = lax.axis_index("tp")
    width = part_refs[0].shape[1]
    squares = 0.0
    product = 0.0
    for mask, ref in zip(masks, part_refs, strict=True):
        at = pl.multiple_of((me ^ mask) * width, width)
        att = ref[...].astype(F32)
        squares = squares + jnp.sum(att * att, axis=1, keepdims=True)
        scaled = (att * gain_ref[:, pl.ds(at, width)]).astype(BF16)
        product = product + jnp.dot(
            scaled, w_ref[pl.ds(at, width), :], preferred_element_type=F32
        )
    inverse = lax.rsqrt(squares / columns + NORM_EPS)
    out_ref[...] = (inverse * product).astype(BF16)


def per_device(tables, tokens, w_query, w_key, w_value, w_out, out_gain, chosen):
    peers = lax.axis_size("kv")
    ways = lax.axis_size("tp")
    rows, depth = tokens.shape
    width = w_query.shape[1]
    names = chosen[0]
    row_table, place_table = (jnp.asarray(t) for t in tables)
    sign = call(sign_kernel, jax.ShapeDtypeStruct((8, LANES), F32), 0, SIGN_FLOPS, mib=1)()
    turns = (row_table, place_table, sign)
    pair_shape = jax.ShapeDtypeStruct((rows, LANES), BF16)
    pairs = call(
        kv_kernel,
        pair_shape,
        6,
        2 * rows * depth * LANES,
        [pltpu.VMEM((LANES, depth), BF16)],
        mib=8,
    )(tokens, w_key.T, w_value.T, *turns)
    q = call(
        query_kernel, jax.ShapeDtypeStruct((rows, width), BF16), 5, 2 * rows * depth * width, mib=8
    )(tokens, w_query, *turns)
    if spread(peers):
        swap = {m: [(i, i ^ m) for i in range(peers)] for m in range(1, peers)}
        far = list(range(peers - 2, 0, -2))
        asked = [chosen]
        for m in far:
            asked.append(lax.ppermute(chosen, "kv", swap[m]))
        beside = lax.ppermute(pairs, "kv", swap[1])
        given = call(
            give_kernel,
            tuple(jax.ShapeDtypeStruct((PAIR, LANES), BF16) for _ in asked),
            len(asked) + 2,
            10**6,
            mib=4,
        )(*asked, pairs, beside)
        arrived = [given[0]]
        for m, blocks in zip(far, given[1:], strict=True):
            arrived.append(lax.ppermute(blocks, "kv", swap[m]))
        masks = (0, *far)
    else:
        table = jnp.broadcast_to(names[None], (peers, *names.shape))
        outgoing = call(
            pick_kernel, jax.ShapeDtypeStruct((peers, BLK, LANES), BF16), 2, 10**6, mib=8
        )(lax.all_to_all(table, "kv", 0, 0, tiled=True), pairs)
        arrived = [lax.all_to_all(outgoing, "kv", 0, 0, tiled=True).reshape(peers * BLK, LANES)]
        masks = ()
    step = rows // CHUNKS
    lse, attended = call(
        local_kernel,
        (
            jax.ShapeDtypeStruct((rows, width), F32),
            jax.ShapeDtypeStruct((rows, width), BF16),
        ),
        3,
        2 * 10**9,
        mib=16,
    )(q, pairs, names)
    flips = [1 << i for i in reversed(range((ways - 1).bit_length()))]
    swaps = {m: [(i, i ^ m) for i in range(ways)] for m in flips}
    gain = out_gain[None, :]
    columns = gain.shape[1]
    cols = w_out.shape[1]
    sent = []
    for c in reversed(range(CHUNKS)):
        mixed = call(
            functools.partial(remote_kernel, c * step, masks),
            jax.ShapeDtypeStruct((step, width), BF16),
            4 + len(arrived),
            10**8,
            [pltpu.VMEM((8, LANES) if masks else (step, width), F32)],
        )(names, q, lse, attended, *arrived)
        sent.append((c, [mixed, lax.ppermute(mixed, "tp", swaps[flips[0]])]))
    result = None
    for c, held in sent:
        masks = [0, flips[0]]
        for m in flips[1:]:
            more = []
            for h in held:
                more.append(lax.ppermute(h, "tp", swaps[m]))
            held = held + more
            masks = masks + [k ^ m for k in masks]
        extra = [] if result is None else [result]
        result = pl.pallas_call(
            functools.partial(out_kernel, columns, masks),
            out_shape=jax.ShapeDtypeStruct((rows, cols), BF16),
            grid=(1,),
            in_specs=[vmem()] * (len(held) + 2)
            + [pl.BlockSpec(memory_space=pl.ANY)] * len(extra),
            out_specs=pl.BlockSpec((step, cols), lambda i, c=c: (c, 0)),
            input_output_aliases={len(held) + 2: 0} if extra else {},
            compiler_params=pltpu.CompilerParams(vmem_limit_bytes=16 * 2**20),
            cost_estimate=pl.CostEstimate(
                flops=2 * step * columns * cols, bytes_accessed=2**20, transcendentals=0
            ),
        )(*held, gain, w_out, *extra)
    return result


def spread(peers):
    return peers <= 16 and peers & (peers - 1) == 0


def solution(mesh):
    def run(tokens, *rest):
        rows = tokens.shape[0] // mesh.shape["kv"]
        tables = rope_tables(rows, mesh.shape["kv"])

        def body(*args):
            return per_device(tables, *args)

        return jax.shard_map(
            body,
            mesh=mesh,
            in_specs=(
                P("kv", None),
                P(None, "tp"),
                P(None, "tp"),
                P(None, "tp"),
                P(None, "tp"),
                P(),
                P("tp", "kv", None),
            ),
            out_specs=P("kv", "tp"),
            check_vma=False,
        )(tokens, *rest)

    return run
```
